128 devices in a mesh: ep: 32 (over z, y, core), tp: 4 (over x).
Axes of the slice: x: 4, y: 4, z: 4, core: 2. Of those that a mesh axis runs over, the one named last changes fastest.
Arguments:
- mixer_input: bfloat16 [16384, 2048], P('ep'), may hold values from -6 to 6
- log_forget_total: float32 [16, 16384], P('tp'), may hold values from -2732 to 0, as said below
- mixer_gain: float32 [2048], replicated, may hold values from 0.1 to 1.9
- w_query: bfloat16 [2048, 1024], P(None, 'tp'), may hold values from -1 to 1
- w_key: bfloat16 [2048, 256], P(None, 'tp'), may hold values from -8 to 8
- w_value: bfloat16 [2048, 256], P(None, 'tp'), may hold values from -0.125 to 0.125
- w_output: bfloat16 [1024, 2048], replicated, may hold values from -0.1875 to 0.1875
- mixer_post_gain: float32 [2048], replicated, may hold values from 0.1 to 1.9
- expert_input: bfloat16 [8192, 2048], P('ep'), may hold values from -6 to 6
- expert_ids: int32 [8192, 2], P('ep'), may hold values from 0 to 31, all different within a row; in each aligned block of 64 rows (0 to 63, 64 to 127, ...) at most 8 rows name the same one
- route_weight: float32 [8192, 2], P('ep'), may hold values from 0.1 to 1
- expert_gain: float32 [2048], replicated, may hold values from 0.1 to 1.9
- w_gate: bfloat16 [32, 2048, 3584], P('ep', None, 'tp'), may hold values from -0.125 to 0.125
- w_up: bfloat16 [32, 2048, 3584], P('ep', None, 'tp'), may hold values from -0.125 to 0.125
- w_down: bfloat16 [32, 3584, 2048], P('ep', 'tp'), may hold values from -0.09375 to 0.09375
- expert_post_gain: float32 [2048], replicated, may hold values from 0.1 to 1.9
Outputs:
- mixer_out: bfloat16 [16384, 2048], P(('ep', 'tp'))
- expert_out: bfloat16 [8192, 2048], P(('ep', 'tp'))
The draws below stay inside these ranges and needn't reach their ends.
Inputs may be any that keep to these rules, and one draw needn't show every extreme that they name: `expert_ids`: in each aligned block of 64 tokens no expert is named by more than 8 of them. `log_forget_total`: each head's values never rise along the positions.
All inputs are finite; a program needn't handle non-finite values.
Results may differ from the reference program's by a relative error of at most 0.012.
The reference program's roundings to bfloat16 on the way count: a program that leaves them out, or rounds other values in their place, can miss the bound.
Values may be sent and summed in bfloat16 or wider, within the bound.
A program may use at most 128 MiB of HBM per device.

```python
import math
import jax
import jax.numpy as jnp
import numpy as np
from jax import lax

D = 2048
QUERY_HEADS = 16
KV_HEADS = 4
HD = 64
FF = 3584
TOP_K = 2
ATT_ROWS = 512
ATTENTION_SPAN = 16384
MOE_TOKENS = 8192
EXPERTS = 32
QROWS = 64
CAPQ = 8
N_EP = 32
N_TP = 4


def draw_mixer_input(key, part):
    drawn = jax.random.normal(jax.random.fold_in(key, 7), (ATTENTION_SPAN, D), jnp.float32)
    return jnp.clip(drawn, -6.0, 6.0).astype(jnp.bfloat16)


def draw_log_forget_total(key, part):
    order = jax.random.permutation(jax.random.fold_in(key, 21), QUERY_HEADS)
    slow_count = QUERY_HEADS // 2
    slow = order < slow_count
    slow_rate = jax.random.uniform(jax.random.fold_in(key, 22), (QUERY_HEADS,), jnp.float32, 0.2, 0.8) / ATTENTION_SPAN
    fast_rate = 1.0 / jax.random.uniform(jax.random.fold_in(key, 23), (QUERY_HEADS,), jnp.float32, 30.0, 100.0)
    step_rate = jnp.where(slow, slow_rate, fast_rate)
    block_factor = jnp.exp(jax.random.uniform(jax.random.fold_in(key, 24), (ATTENTION_SPAN // ATT_ROWS, QUERY_HEADS), jnp.float32, math.log(0.4), math.log(2.5)))
    per_position = jnp.repeat(block_factor, ATT_ROWS, axis=0)
    rough = jax.random.uniform(jax.random.fold_in(key, 25), (ATTENTION_SPAN, QUERY_HEADS), jnp.float32, 0.3, 1.7)
    gate_logarithm = -step_rate[None, :] * per_position * rough
    spike_position = jax.random.randint(jax.random.fold_in(key, 26), (3,), 0, ATTENTION_SPAN)
    spike_length = jnp.log(jax.random.uniform(jax.random.fold_in(key, 27), (3, QUERY_HEADS), jnp.float32, 0.6, 0.8))
    match_count = (jnp.arange(ATTENTION_SPAN)[:, None] == spike_position[None, :]).astype(jnp.float32)
    gate_logarithm = gate_logarithm + jnp.sum(match_count[:, :, None] * spike_length[None, :, :], axis=1)
    return jnp.transpose(jnp.cumsum(gate_logarithm, axis=0))


def query_key_pair(key):
    query_w = jax.random.normal(jax.random.fold_in(key, 31), (D, QUERY_HEADS * HD), jnp.float32) * D ** (-0.5)
    key_w = jax.random.normal(jax.random.fold_in(key, 32), (D, KV_HEADS * HD), jnp.float32) * D ** (-0.5)
    return (jnp.clip(query_w, -1.0, 1.0), jnp.clip(key_w, -8.0, 8.0))


def draw_w_query(key, part):
    return query_key_pair(key)[0].astype(jnp.bfloat16)


def draw_w_key(key, part):
    return query_key_pair(key)[1].astype(jnp.bfloat16)


def level_of(key, extent, split, smallest, top_value):
    def one(axis_at, parts):
        heights = jax.random.uniform(jax.random.fold_in(jax.random.fold_in(key, 6), axis_at), (parts,), jnp.float32, smallest / len(split), top_value / len(split))
        return jnp.repeat(jnp.exp(heights), extent[axis_at] // parts).reshape((-1,) + (1,) * (len(extent) - axis_at - 1))

    loudness = one(*split[0])
    for cut in split[1:]:
        loudness = loudness * one(*cut)
    return loudness


def deal_out(rng, own, number, rows, number_of, top, bound, skew):
    order = jax.random.permutation(rng, number_of)
    heavy_load, usual = portions_of(number_of, rows * top, bound, skew, True), portions_of(number_of, rows * top, bound, skew, False)
    places = jnp.arange(number_of)

    def named(tallies, turn):
        used = int((tallies > 0).sum())
        fixed = max(1, used // 4)
        moved = fixed + (places - fixed + turn * (used - fixed)) % max(1, number_of - fixed)
        return jnp.zeros((number_of,), jnp.int32).at[order[jnp.where(places < fixed, places, moved)]].set(jnp.asarray(tallies, jnp.int32))

    tallies = jnp.where(number % 4 == 0, named(heavy_load, number // 4), named(usual, number - number // 4 - 1))
    mixed = jax.random.permutation(jax.random.fold_in(own, 3), number_of)
    source_of, receiver = mixed[0:number_of // 2 * 2:2], mixed[1:number_of // 2 * 2:2]
    margin = jnp.minimum(tallies[source_of] - 1, bound - tallies[receiver]) // 2
    margin = jnp.where((source_of == order[0]) | (receiver == order[0]) | (tallies[receiver] == 0), 0, jnp.maximum(margin, 0))
    moved = jax.random.randint(jax.random.fold_in(own, 4), (number_of // 2,), 0, 1 << 20) % (margin + 1)
    tallies = tallies.at[source_of].add(-moved).at[receiver].add(moved)
    items = jnp.searchsorted(jnp.cumsum(tallies), jnp.arange(rows * top), side="right").astype(jnp.int32)
    listing = items.reshape(top, rows).T
    listing = listing[jax.random.permutation(jax.random.fold_in(own, 1), rows)]
    turn = jax.random.randint(jax.random.fold_in(own, 2), (rows, 1), 0, top)
    return jnp.take_along_axis(listing, (jnp.arange(top)[None, :] + turn) % top, axis=1)


def portions_of(amount, total, reach, slope, full):
    weights = [(1 << 20) // math.isqrt(rank ** slope) + 1 for rank in range(1, amount + 1)]
    largest = reach if full else min(reach, max(-(-total // amount), total * weights[0] // sum(weights)))
    least = 1 if total - largest >= amount - 1 else 0
    counts, rest = [largest] + [least] * (amount - 1), total - largest - least * (amount - 1)
    while rest > 0:
        candidates = [i for i in range(1, amount) if counts[i] < largest] or [i for i in range(1, amount) if counts[i] < reach]
        mass, left = sum([weights[i] for i in candidates]), rest
        for i in candidates:
            addition = min(reach - counts[i], max(1, left * weights[i] // mass), rest)
            counts[i] = counts[i] + addition
            rest = rest - addition
    return np.array(counts)


def scatter_about(own_key, shape, scale, reach, split=(), held_as=jnp.bfloat16):
    gain = level_of(own_key, shape, split, -0.22, 0.18) if split else 1.0
    entries = jax.random.normal(own_key, shape, jnp.float32) * scale * gain
    return jnp.minimum(jnp.maximum(entries, -reach), reach).astype(held_as)


def setup_inputs(seed: int = 0) -> dict:
    seeds = jax.random.split(jax.random.key(seed), 17)
    mixer_input = draw_mixer_input(jax.random.fold_in(seeds[16], 71), 0)
    log_forget_total = draw_log_forget_total(jax.random.fold_in(seeds[16], 71), 0)
    mixer_gain = jnp.clip(1.0 + 0.18 * jax.random.normal(seeds[2], (D,), jnp.float32), 0.1, 1.9)
    w_query = draw_w_query(jax.random.fold_in(seeds[16], 71), 0)
    w_key = draw_w_key(jax.random.fold_in(seeds[16], 71), 0)
    w_value = scatter_about(seeds[5], (D, KV_HEADS * HD), D ** -0.5, 0.125, ((1, 4),))
    w_output = scatter_about(seeds[6], (QUERY_HEADS * HD, D), (QUERY_HEADS * HD) ** -0.5, 0.1875)
    mixer_post_gain = jnp.clip(1.0 + 0.18 * jax.random.normal(seeds[7], (D,), jnp.float32), 0.1, 1.9)
    expert_input = scatter_about(seeds[8], (MOE_TOKENS, D), 1.0, 6.0, ((0, 32),))
    expert_ids_keys = jax.random.split(jax.random.fold_in(seeds[9], 1), MOE_TOKENS // QROWS)
    expert_ids_turns = jax.random.permutation(jax.random.fold_in(seeds[9], 3), MOE_TOKENS // QROWS)
    expert_ids = jax.vmap(lambda own, number: deal_out(jax.random.fold_in(seeds[9], 2), own, number, QROWS, EXPERTS, TOP_K, CAPQ, 2))(expert_ids_keys, expert_ids_turns).reshape((MOE_TOKENS, TOP_K))
    route_weight = jnp.clip(jnp.exp(math.log(1.0) - 2.3025851 * jax.random.uniform(seeds[10], (MOE_TOKENS, TOP_K), jnp.float32) ** level_of(seeds[10], (MOE_TOKENS, TOP_K), ((0, 32),), -0.2, 0.2)), 0.1, 1.0)
    expert_gain = jnp.clip(1.0 + 0.18 * jax.random.normal(seeds[11], (D,), jnp.float32), 0.1, 1.9)
    w_gate = scatter_about(seeds[12], (EXPERTS, D, FF), D ** -0.5, 0.125, ((0, 32), (2, 4)))
    w_up = scatter_about(seeds[13], (EXPERTS, D, FF), D ** -0.5, 0.125, ((0, 32), (2, 4)))
    w_down = scatter_about(seeds[14], (EXPERTS, FF, D), FF ** -0.5, 0.09375, ((0, 32), (1, 4)))
    expert_post_gain = jnp.clip(1.0 + 0.18 * jax.random.normal(seeds[15], (D,), jnp.float32), 0.1, 1.9)
    return {"mixer_input": mixer_input, "log_forget_total": log_forget_total, "mixer_gain": mixer_gain, "w_query": w_query, "w_key": w_key, "w_value": w_value, "w_output": w_output, "mixer_post_gain": mixer_post_gain, "expert_input": expert_input, "expert_ids": expert_ids, "route_weight": route_weight, "expert_gain": expert_gain, "w_gate": w_gate, "w_up": w_up, "w_down": w_down, "expert_post_gain": expert_post_gain}


NEG_FILL = -1e+30
NORM_EPS = 1e-06

def norm_rows(values_in, gain_vec):
    widened = values_in.astype(jnp.float32)
    return widened * lax.rsqrt(lax.optimization_barrier(jnp.mean(widened * widened, axis=-1, keepdims=True)) + NORM_EPS) * gain_vec.astype(jnp.float32)

def rounded(values_in):
    return lax.optimization_barrier(values_in.astype(jnp.bfloat16))

def mixer_part(mixer_input, log_forget_total, mixer_gain, w_query, w_key, w_value, w_output, mixer_post_gain):
    normed = rounded(norm_rows(mixer_input, mixer_gain))
    queries = rounded(jnp.dot(normed, w_query, preferred_element_type=jnp.float32))
    key_rows = rounded(jnp.dot(normed, w_key, preferred_element_type=jnp.float32))
    value_rows = rounded(jnp.dot(normed, w_value, preferred_element_type=jnp.float32))
    group_size = QUERY_HEADS // KV_HEADS
    block_rows = math.gcd(ATTENTION_SPAN, 512)
    block_total = ATTENTION_SPAN // block_rows
    query_blocks = queries.reshape(block_total, block_rows, KV_HEADS, group_size, HD)
    key_wide = key_rows.astype(jnp.float32).reshape(ATTENTION_SPAN, KV_HEADS, HD)
    value_wide = value_rows.astype(jnp.float32).reshape(ATTENTION_SPAN, KV_HEADS, HD)
    gate_totals = log_forget_total.astype(jnp.float32).reshape(KV_HEADS, group_size, ATTENTION_SPAN)
    positions = jnp.arange(ATTENTION_SPAN, dtype=jnp.int32)
    score_scale = HD ** (-0.5)

    def one_block(operands):
        query_block, block_index = operands
        first_row = (block_index * block_rows).astype(jnp.int32)
        query_pos = first_row + jnp.arange(block_rows, dtype=jnp.int32)
        visible = positions[None, :] <= query_pos[:, None]
        outputs = []
        for head_group in range(KV_HEADS):
            group_gates = gate_totals[head_group]
            query_gate = lax.dynamic_slice_in_dim(group_gates, first_row, block_rows, 1)
            scores = jnp.einsum('qjd,kd->jqk', query_block[:, head_group].astype(jnp.float32), key_wide[:, head_group]) * score_scale
            scores = scores + query_gate[:, :, None] - group_gates[:, None, :]
            scores = jnp.where(visible[None], scores, NEG_FILL)
            row_max = lax.optimization_barrier(jnp.max(scores, axis=-1, keepdims=True))
            shifted = jnp.where(visible[None], jnp.exp(scores - row_max), 0.0)
            denominator = lax.optimization_barrier(jnp.sum(shifted, axis=-1))
            weights = rounded(shifted).astype(jnp.float32)
            numerator = jnp.einsum('jqk,kd->qjd', weights, value_wide[:, head_group])
            outputs.append(numerator / jnp.transpose(denominator)[:, :, None])
        return rounded(jnp.concatenate(outputs, axis=1).reshape(block_rows, QUERY_HEADS * HD))
    mixed_heads = lax.map(one_block, (query_blocks, jnp.arange(block_total, dtype=jnp.int32)))
    mixed_heads = mixed_heads.reshape(ATTENTION_SPAN, QUERY_HEADS * HD)
    projected = jnp.dot(mixed_heads, w_output, preferred_element_type=jnp.float32)
    return norm_rows(projected, mixer_post_gain).astype(jnp.bfloat16)

def expert_part(expert_input, expert_ids, route_weight, expert_gain, w_gate, w_up, w_down, expert_post_gain):
    normed = rounded(norm_rows(expert_input, expert_gain))
    assigned = MOE_TOKENS * TOP_K
    capacity = N_EP * N_TP * CAPQ
    group_units = FF // N_TP
    flat_ids = expert_ids.reshape(assigned)
    owners = jnp.concatenate([jnp.arange(assigned, dtype=jnp.int32) // TOP_K, jnp.full((1,), MOE_TOKENS, jnp.int32)])
    shares = jnp.concatenate([route_weight.reshape(assigned).astype(jnp.float32), jnp.zeros((1,), jnp.float32)])
    padded_rows = jnp.concatenate([normed, jnp.zeros((1, D), jnp.bfloat16)], axis=0)

    def one_expert(running, expert):
        chosen = flat_ids == expert
        slot_ranks = jnp.cumsum(chosen.astype(jnp.int32)) - 1
        slot_target = jnp.where(chosen, slot_ranks, capacity).astype(jnp.int32)
        slot_table = jnp.full((capacity,), assigned, jnp.int32).at[slot_target].set(jnp.arange(assigned, dtype=jnp.int32), mode='drop')
        token_rows = owners[slot_table]
        inputs = padded_rows[token_rows]
        gate_part = jnp.dot(inputs, w_gate[expert], preferred_element_type=jnp.float32)
        up_part = jnp.dot(inputs, w_up[expert], preferred_element_type=jnp.float32)
        hidden = rounded(jax.nn.silu(gate_part) * up_part)
        down_local = w_down[expert]
        summed = jnp.zeros((capacity, D), jnp.float32)
        for group_index in range(N_TP):
            low_unit = group_index * group_units
            group_term = jnp.dot(hidden[:, low_unit:low_unit + group_units], down_local[low_unit:low_unit + group_units], preferred_element_type=jnp.float32)
            summed = summed + rounded(group_term).astype(jnp.float32)
        expert_rows = rounded(summed).astype(jnp.float32)
        running = running.at[token_rows].add(shares[slot_table][:, None] * expert_rows, mode='drop')
        return (running, None)
    combined, _ = lax.scan(one_expert, jnp.zeros((MOE_TOKENS, D), jnp.float32), jnp.arange(EXPERTS, dtype=jnp.int32))
    return norm_rows(combined, expert_post_gain).astype(jnp.bfloat16)

def reference(mixer_input, log_forget_total, mixer_gain, w_query, w_key, w_value, w_output, mixer_post_gain, expert_input, expert_ids, route_weight, expert_gain, w_gate, w_up, w_down, expert_post_gain):
    mixer_out = mixer_part(mixer_input, log_forget_total, mixer_gain, w_query, w_key, w_value, w_output, mixer_post_gain)
    expert_out = expert_part(expert_input, expert_ids, route_weight, expert_gain, w_gate, w_up, w_down, expert_post_gain)
    return (mixer_out, expert_out)
```

```python
import functools
import math

import jax
import jax.numpy as jnp
from jax import lax
from jax.experimental import pallas as pl
from jax.experimental.pallas import tpu as pltpu
from jax.sharding import PartitionSpec as P

HD = 64
TOP_K = 2
NEG_FILL = -1e30
NORM_EPS = 1e-06
F32 = jnp.float32
BF16 = jnp.bfloat16


def norm_rows(values_in, gain_vec):
    widened = values_in.astype(F32)
    return (
        widened
        * lax.rsqrt(jnp.mean(widened * widened, axis=-1, keepdims=True) + NORM_EPS)
        * gain_vec
    )


def dot(a, b):
    return jnp.dot(a, b, preferred_element_type=F32)


def attention_kernel(n_ep, heads, half, kv_ref, g_ref, qt_ref, o_ref, qs, m_s, l_s, acc):
    me = lax.axis_index("ep")
    other = n_ep - 1 - me
    nq = heads * half
    row = lax.broadcasted_iota(jnp.int32, (128, nq), 0)
    col = lax.broadcasted_iota(jnp.int32, (128, nq), 1)
    sel = jnp.where((row < 3 * heads) & (row % heads == col // half), 1.0, 0.0).astype(BF16)
    zero = jnp.zeros((HD, nq), BF16)
    for hf in range(2):
        q = qt_ref[hf]
        qs[hf, 0] = jnp.concatenate([q, zero, sel], axis=0)
        qs[hf, 1] = jnp.concatenate([zero, q, sel], axis=0)
    m_s[...] = jnp.full(m_s.shape, NEG_FILL, F32)
    l_s[...] = jnp.zeros(l_s.shape, F32)
    acc[...] = jnp.zeros(acc.shape, F32)
    hidden = lax.broadcasted_iota(jnp.int32, (half, half), 0) > lax.broadcasted_iota(
        jnp.int32, (half, half), 1
    )

    def step(hf, kb, mode):
        kp = kv_ref[kb, 0:half, :]
        parts = [0] if mode == "first" else [0, 1]
        keys = [
            jnp.concatenate([kp, g_ref[kb, pt * half : (pt + 1) * half, :]], axis=1) for pt in parts
        ]
        vt = jnp.concatenate(
            [kv_ref[kb, half + HD * c : half + HD * (c + 1), :] for c in range(2 * len(parts))], axis=1
        )
        for h in range(heads):
            cols = slice(h * half, (h + 1) * half)
            sc = [dot(keys[pt], qs[hf, pt, :, cols]) for pt in parts]
            if mode != "full":
                sc[-1] = jnp.where(hidden, NEG_FILL, sc[-1])
            top = m_s[hf, 0:1, cols]
            new = top
            for s in sc:
                new = jnp.maximum(new, jnp.max(s, axis=0, keepdims=True))
            ps = [jnp.exp(s - new) for s in sc]
            factor = jnp.exp(top - new)
            den = l_s[hf, 0:1, cols] * factor
            for p in ps:
                den = den + jnp.sum(p, axis=0, keepdims=True)
            l_s[hf, 0:1, cols] = den
            m_s[hf, 0:1, cols] = new
            pb = jnp.concatenate([p.astype(BF16) for p in ps], axis=0)
            acc[hf, :, cols] = acc[hf, :, cols] * factor + dot(vt, pb)

    @pl.loop(0, me)
    def _(kb):
        step(0, kb, "full")

    step(0, me, "first")

    @pl.loop(0, other)
    def _(kb):
        step(1, kb, "full")

    step(1, other, "second")
    for hf in range(2):
        o_ref[hf] = (acc[hf] / l_s[hf, 0:1, :]).astype(BF16)


def attention(kv, gates, qt, n_ep, heads, half):
    nq = heads * half
    return pl.pallas_call(
        functools.partial(attention_kernel, n_ep, heads, half),
        out_shape=jax.ShapeDtypeStruct((2, HD, nq), BF16),
        in_specs=[pl.BlockSpec(memory_space=pltpu.VMEM)] * 3,
        out_specs=pl.BlockSpec(memory_space=pltpu.VMEM),
        scratch_shapes=[
            pltpu.VMEM((2, 2, 256, nq), BF16),
            pltpu.VMEM((2, 8, nq), F32),
            pltpu.VMEM((2, 8, nq), F32),
            pltpu.VMEM((2, HD, nq), F32),
        ],
        compiler_params=pltpu.CompilerParams(vmem_limit_bytes=48 * 1024 * 1024),
        cost_estimate=pl.CostEstimate(
            flops=30_000_000_000, bytes_accessed=9_000_000, transcendentals=17_000_000
        ),
        name="attention",
    )(kv, gates, qt)


def pieces_of(values):
    out, rest = [], values
    for _ in range(3):
        piece = lax.reduce_precision(rest, 8, 7)
        out.append(piece.astype(BF16))
        rest = rest - piece
    return out


def mixer_half(
    mixer_input, log_forget_total, mixer_gain, w_query, w_key, w_value, w_output, mixer_post_gain
):
    rows = mixer_input.shape[0]
    half = rows // 2
    heads = w_query.shape[1] // HD
    n_ep = lax.axis_size("ep")
    normed = norm_rows(mixer_input, mixer_gain).astype(BF16)
    queries = dot(normed, w_query).astype(BF16)
    keys = dot(normed, w_key).astype(BF16)
    values = dot(normed, w_value).astype(BF16)
    packed_keys = jnp.concatenate([keys[:half], keys[half:]], axis=1)
    values_t = values.T.reshape(HD, rows // 128, 128).transpose(1, 0, 2).reshape(half, 128)
    kv_own = jnp.concatenate([packed_keys, values_t], axis=0)
    kv = lax.all_gather(kv_own, "ep", axis=0, tiled=False)
    gates = jnp.concatenate(pieces_of(-log_forget_total), axis=0)
    gates = jnp.pad(gates.T, ((0, 0), (0, 128 - gates.shape[0]))).reshape(n_ep, rows, 128)
    swap = [(i, n_ep - 1 - i) for i in range(n_ep)]
    qt = (queries * BF16(HD**-0.5)).reshape(2, half, heads, HD).transpose(0, 3, 2, 1)
    qt = qt.reshape(2, HD, heads * half)
    far = lax.ppermute(qt[1], "ep", swap)
    out = attention(kv, gates, jnp.stack([qt[0], far]), n_ep, heads, half)
    far_out = lax.ppermute(out[1], "ep", swap)
    mixed = jnp.stack([out[0], far_out]).reshape(2, HD, heads, half)
    mixed_heads = mixed.transpose(0, 3, 2, 1).reshape(rows, heads * HD)
    by_rows = lax.all_to_all(mixed_heads, "tp", split_axis=0, concat_axis=1, tiled=True)
    projected = dot(by_rows, w_output)
    return norm_rows(projected, mixer_post_gain).astype(BF16)


def expert_half(
    expert_input, expert_ids, route_weight, expert_gain, w_gate, w_up, w_down, expert_post_gain
):
    row_count, width = expert_input.shape
    quarters = lax.axis_size("tp")
    experts = lax.axis_size("ep")
    quarter_rows = row_count // quarters
    slots = 2 * TOP_K * quarter_rows // experts
    own_quarter = lax.axis_index("tp")
    normed = norm_rows(expert_input, expert_gain).astype(BF16)
    ids = expert_ids.reshape(quarters, quarter_rows, TOP_K)
    each = jnp.arange(experts, dtype=jnp.int32)
    chosen = jnp.any(ids[..., None] == each, axis=2)
    before = jnp.tril(jnp.ones((quarter_rows, quarter_rows), BF16), -1)
    ranks = jnp.einsum(
        "ut,bte->bue", before, chosen.astype(BF16), preferred_element_type=F32
    ).astype(jnp.int32)
    ranks = jnp.where(chosen, ranks, -1)
    table = (ranks[..., None] == jnp.arange(slots, dtype=jnp.int32)).astype(BF16)
    table = table.reshape(quarters, quarter_rows, experts * slots)
    outgoing = jnp.einsum(
        "bts,btd->bsd",
        table,
        normed.reshape(quarters, quarter_rows, width),
        preferred_element_type=F32,
    ).astype(BF16)
    outgoing = outgoing.reshape(quarters, experts, slots, width)
    arrived = lax.all_to_all(outgoing, "ep", split_axis=1, concat_axis=1, tiled=True)
    flat_rows = arrived.reshape(-1, width)
    gate_part = dot(flat_rows, w_gate[0])
    up_part = dot(flat_rows, w_up[0])
    hidden = (jax.nn.silu(gate_part) * up_part).astype(BF16)
    product = dot(hidden, w_down[0]).astype(BF16)
    summed = lax.psum_scatter(
        product.reshape(quarters, experts, slots, width), "tp", scatter_dimension=0, tiled=True
    )
    returned = lax.all_to_all(summed[0], "ep", split_axis=0, concat_axis=0, tiled=True)
    flat_results = returned.reshape(experts * slots, width)
    own_table = lax.dynamic_index_in_dim(table, own_quarter, 0, keepdims=False)
    own_table = own_table.reshape(quarter_rows, experts, slots)
    own_ids = lax.dynamic_index_in_dim(ids, own_quarter, 0, keepdims=False)
    own_weights = lax.dynamic_slice_in_dim(
        route_weight, own_quarter * quarter_rows, quarter_rows, 0
    )
    combined = jnp.zeros((quarter_rows, width), F32)
    for k in range(TOP_K):
        mine = (own_ids[:, k, None] == each).astype(BF16)[:, :, None]
        picked = dot((own_table * mine).reshape(quarter_rows, -1), flat_results)
        combined = combined + own_weights[:, k, None] * picked
    return norm_rows(combined, expert_post_gain).astype(BF16)


def per_device(*args):
    return (mixer_half(*args[:8]), expert_half(*args[8:]))


def solution(mesh):
    placed = (
        P("ep", None),
        P("tp", None),
        P(),
        P(None, "tp"),
        P(None, "tp"),
        P(None, "tp"),
        P(),
        P(),
        P("ep", None),
        P("ep", None),
        P("ep", None),
        P(),
        P("ep", None, "tp"),
        P("ep", None, "tp"),
        P("ep", "tp", None),
        P(),
    )
    return jax.shard_map(
        per_device,
        mesh=mesh,
        in_specs=placed,
        out_specs=(P(("ep", "tp"), None), P(("ep", "tp"), None)),
        check_vma=False,
    )
```

```python
import functools

import jax
import jax.numpy as jnp
from jax import lax
from jax.experimental import pallas as pl
from jax.experimental.pallas import tpu as pltpu
from jax.sharding import PartitionSpec as P

HD = 64
TOP_K = 2
NEG_FILL = -1e30
NORM_EPS = 1e-06
F32 = jnp.float32
BF16 = jnp.bfloat16
SLOT = 8


def norm_rows(values_in, gain_vec):
    widened = values_in.astype(F32)
    return (
        widened
        * lax.rsqrt(jnp.mean(widened * widened, axis=-1, keepdims=True) + NORM_EPS)
        * gain_vec
    )


def dot(a, b):
    return jnp.dot(a, b, preferred_element_type=F32)


def dot_t(a, b):
    return lax.dot_general(a, b, (((0,), (0,)), ((), ())), preferred_element_type=F32)


def iota(shape, dim):
    return lax.broadcasted_iota(jnp.int32, shape, dim)


def whole_kernel(
    x_ref, lf_ref, again_ref, wq_ref, wk_ref, wv_ref, wo_hbm, apost_ref,
    m_ref, ids_ref, rw_ref, mgain_ref, wg_hbm, wu_hbm, wd_hbm, mpost_ref,
    mix_out, exp_out,
    wg, wu, wd, wo, w_sem,
    outgoing, arr, prod, own, far_s, far_r, near_s, near_r, res, ret,
    kv, qo, qf, gs, qs, m_s, acc, s_a, s_b, ob, mx,
    disp_ss, disp_rs, fwd_ss, fwd_rs, far_ss, far_rs, near_ss, near_rs, ret_ss, ret_rs,
    q_sem, k1_ss, k1_rs, k2_ss, k2_rs, k3_ss, k3_rs, ob_ss, ob_rs,
):
    me = lax.axis_index("ep")
    p = lax.axis_index("tp")
    z, y, c = me // 8, (me // 2) % 4, me % 2
    mirror = 31 - me
    parity = p % 2
    rows = x_ref.shape[0]
    half = rows // 2
    heads = wq_ref.shape[1] // HD
    nq = heads * half
    width = x_ref.shape[1]
    tokens = m_ref.shape[0]
    quarter = tokens // 4
    experts = arr.shape[1]
    upper = experts // 2

    def ep_of(a, b, d):
        return ((a + 8) % 4) * 8 + ((b + 8) % 4) * 2 + (d + 2) % 2

    def away(r, sign):
        g, j, d = r // 8, (r // 2) % 4, r % 2
        return ep_of(z + sign * j, y + sign * (g + j), c + d)

    def send(src, dst, s_sem, r_sem, ep, tp):
        return pltpu.make_async_remote_copy(
            src_ref=src,
            dst_ref=dst,
            send_sem=s_sem,
            recv_sem=r_sem,
            device_id={"ep": ep, "tp": tp},
            device_id_type=pl.DeviceIdType.MESH,
        )

    weights = [
        pltpu.make_async_copy(a, b, w_sem.at[k])
        for k, (a, b) in enumerate(((wg_hbm.at[0], wg), (wu_hbm.at[0], wu), (wd_hbm.at[0], wd), (wo_hbm, wo)))
    ]
    for w in weights:
        w.start()

    normed_m = norm_rows(m_ref[...], mgain_ref[...]).astype(BF16)
    each = iota((tokens, experts), 1)
    chosen = ((ids_ref[:, 0:1] == each) | (ids_ref[:, 1:2] == each)).astype(F32).astype(BF16)
    t_row, t_col = iota((tokens, tokens), 0), iota((tokens, tokens), 1)
    before = ((t_row // quarter == t_col // quarter) & (t_row < t_col)).astype(F32).astype(BF16)
    same = (t_row == t_col).astype(F32).astype(BF16)
    chosen_t = dot_t(chosen, same)
    ranks_t = dot_t(chosen, before)
    ranks_t = jnp.where(chosen_t > 0.5, ranks_t, -1.0)
    block_of = iota((experts, tokens), 1) // quarter
    for hb in range(2):
        mine = jnp.where(block_of == parity + 2 * hb, ranks_t, -1.0)
        wide = jnp.broadcast_to(mine[:, None, :], (experts, SLOT, tokens))
        table = jnp.where(wide == iota((experts, SLOT, tokens), 1).astype(F32), 1.0, 0.0)
        table = table.reshape(experts * SLOT, tokens).astype(BF16)
        picked = dot(table, normed_m)
        outgoing[:, hb] = picked.reshape(experts, SLOT, width).astype(BF16)

    def disp(r, peer):
        return send(outgoing.at[peer], arr.at[0, r], disp_ss.at[r], disp_rs.at[r], peer, p)

    def fwd(r):
        return send(
            arr.at[0, r], arr.at[1, r], fwd_ss.at[r], fwd_rs.at[r], me, (p + 1 + 2 * (r % 2)) % 4
        )

    @pl.loop(1, experts)
    def _(r):
        disp(r, away(r, 1)).start()

    arr[0, 0] = outgoing[me]

    normed_a = norm_rows(x_ref[...], again_ref[...]).astype(BF16)
    kt = dot(normed_a, wk_ref[...]).astype(BF16).astype(F32)
    vt = dot(normed_a, wv_ref[...]).astype(BF16).astype(F32)
    kv[me] = jnp.transpose(jnp.concatenate([kt, vt], axis=1)).astype(BF16)
    qt = dot(normed_a, wq_ref[...]).astype(BF16).astype(F32) * (HD**-0.5)
    qt = jnp.transpose(qt).astype(BF16)
    for hf in range(2):
        for h in range(heads):
            qo[hf, :, h * half : (h + 1) * half] = qt[
                h * HD : (h + 1) * HD, hf * half : (hf + 1) * half
            ]
    swap = send(qo.at[1], qf, q_sem.at[0], q_sem.at[1], mirror, p)
    swap.start()

    def first(part, d):
        ref = kv.at[me, part * HD : (part + 1) * HD]
        to = ep_of(z + d, y, c) if part == 0 else ep_of(z, y + d, c)
        return send(ref, ref, k1_ss.at[part, d], k1_rs.at[part, d], to, p)

    def second(part, a, d):
        owner = ep_of(z - a, y, c) if part == 0 else ep_of(z, y - a, c)
        to = ep_of(z, y + d, c) if part == 0 else ep_of(z + d, y, c)
        ref = kv.at[owner, part * HD : (part + 1) * HD]
        return send(ref, ref, k2_ss.at[part, a, d], k2_rs.at[part, a, d], to, p)

    def third(k):
        ref = kv.at[ep_of(z - k // 4, y - k % 4, c)]
        return send(ref, ref, k3_ss.at[k], k3_rs.at[k], ep_of(z, y, c + 1), p)

    for part in range(2):
        for d in range(1, 4):
            first(part, d).start()

    @pl.loop(0, experts)
    def _(kb):
        rest = -lf_ref[:, pl.ds(pl.multiple_of(kb * rows, rows), rows)]
        for k in range(3):
            piece = rest.astype(BF16).astype(F32)
            gs[kb, k * heads : (k + 1) * heads, :] = piece
            rest = rest - piece
        gs[kb, 3 * heads : 16, :] = jnp.zeros((16 - 3 * heads, rows), F32)

    fwd(0).start()

    @pl.loop(1, experts)
    def _(r):
        disp(r, away(r, 1)).wait_recv()
        fwd(r).start()

    for w in weights[:3]:
        w.wait()

    def ffn(v, u):
        rows_in = arr[v, pl.ds(u * upper, upper)].reshape(upper * 2 * SLOT, width)
        gate = dot(rows_in, wg[...])
        up = dot(rows_in, wu[...])
        hidden = (gate / (1.0 + jnp.exp(-gate)) * up).astype(BF16)
        tile = 512

        for n in range(width // tile):
            prod[:, :, :, n * tile : (n + 1) * tile] = dot(
                hidden, wd[:, n * tile : (n + 1) * tile]
            ).reshape(upper, 2, SLOT, tile)

    def far(u):
        return send(
            far_s.at[u], far_r.at[u], far_ss.at[u], far_rs.at[u], me, (p + 1 + 2 * u) % 4
        )

    @pl.loop(0, 2)
    def _(u):
        ffn(0, u)
        own[pl.ds(u * upper, upper)] = prod[:, p // 2].astype(BF16)
        far_s[u] = prod[:, 1 - p // 2].astype(BF16)
        far(u).start()

    for part in range(2):
        for a in range(4):
            if a > 0:
                first(part, a).wait_recv()
            for d in range(1, 4):
                second(part, a, d).start()

    plus = ((p + 1) % 4) // 2

    def near(u, k):
        side = (u + k) % 2
        return send(
            near_s.at[u, k],
            near_r.at[side, pl.ds(u * upper, upper)],
            near_ss.at[u, side],
            near_rs.at[u, side],
            me,
            (p + 1 + 2 * side) % 4,
        )

    @pl.loop(0, 2)
    def _(u):
        @pl.loop(0, upper)
        def _(k):
            fwd(u * upper + k).wait_recv()

        ffn(1, u)
        far(u).wait_recv()
        joined = (plus + u) % 2
        near_s[u, 0] = (
            prod[:, joined].astype(BF16).astype(F32) + far_r[u].astype(F32)
        ).astype(BF16)
        near_s[u, 1] = prod[:, 1 - joined].astype(BF16)
        near(u, 0).start()
        near(u, 1).start()

    third(0).start()
    for a in range(4):
        for b in range(4):
            if (a, b) != (0, 0):
                if b > 0:
                    second(0, a, b).wait_recv()
                if a > 0:
                    second(1, b, a).wait_recv()
                third(a * 4 + b).start()
    swap.wait_recv()
    for k in range(16):
        third(k).wait_recv()

    row, col = iota((16, nq), 0), iota((16, nq), 1)
    sel = jnp.where((row < 3 * heads) & (row % heads == col // half), 1.0, 0.0).astype(BF16)
    qs[0] = jnp.concatenate([qo[0], sel], axis=0)
    qs[1] = jnp.concatenate([qf[...], sel], axis=0)
    m_s[...] = jnp.full(m_s.shape, NEG_FILL, F32)
    acc[...] = jnp.zeros(acc.shape, F32)
    hidden_keys = iota((half, half), 0) > iota((half, half), 1)

    def place(n):
        late = n >= me
        return jnp.where(late, 1, 0), jnp.where(late, n - me, n)

    def scores(hf, kb, s_ref, mode="full"):
        keys = jnp.concatenate([kv[kb, 0:HD, :].astype(F32), gs[kb]], axis=0)
        keys = jnp.transpose(keys).astype(BF16)
        for pt in [0] if mode == "first" else [0, 1]:
            for h in range(heads):
                cols = slice(h * half, (h + 1) * half)
                s = dot(keys[pt * half : (pt + 1) * half], qs[hf, :, cols])
                if mode == "first" or (mode == "second" and pt == 1):
                    s = jnp.where(hidden_keys, NEG_FILL, s)
                s_ref[pt * half : (pt + 1) * half, cols] = s

    def weigh(hf, kb, s_ref, mode="full"):
        count = half if mode == "first" else 2 * half
        vals = jnp.concatenate([kv[kb, HD : 2 * HD, 0:count], jnp.ones((16, count), BF16)], axis=0)
        for h in range(heads):
            cols = slice(h * half, (h + 1) * half)
            top = m_s[hf, 0:1, cols]
            new = jnp.maximum(top, jnp.max(s_ref[0:count, cols], axis=0, keepdims=True))
            weight = jnp.exp(s_ref[0:count, cols] - new).astype(BF16)
            m_s[hf, 0:1, cols] = new
            acc[hf, :, cols] = acc[hf, :, cols] * jnp.exp(top - new) + dot(vals, weight)

    scores(0, me, s_a, "first")
    scores(1, mirror, s_b, "second")
    weigh(0, me, s_a, "first")
    scores(*place(0), s_a)
    weigh(1, mirror, s_b, "second")

    def attend(t):
        n = 2 * t
        scores(*place(n + 1), s_b)
        weigh(*place(n), s_a)
        scores(*place(n + 2), s_a)
        weigh(*place(n + 1), s_b)

    pl.loop(0, (experts - 2) // 2)(attend)
    weigh(*place(experts - 2), s_a)

    for hf in range(2):
        o = (acc[hf, 0:HD, :] / acc[hf, HD : HD + 1, :]).astype(BF16)
        for q in range(2):
            for h in range(heads):
                ob[hf, q, h * HD : (h + 1) * HD, :] = o[
                    :, h * half + q * (half // 2) : h * half + (q + 1) * (half // 2)
                ]

    def deliver(hf, q):
        return send(
            ob.at[hf, q], mx.at[p], ob_ss.at[hf, q], ob_rs.at[p], me if hf == 0 else mirror, 2 * hf + q
        )

    for q in range(2):
        deliver(1, q).start()

        @pl.when(p == q)
        def _():
            mx[q] = ob[0, q]

        @pl.when(p != q)
        def _():
            deliver(0, q).start()

    def give(r):
        return send(res.at[r], ret.at[me], ret_ss.at[r], ret_rs.at[r], away(r, -1), p)

    @pl.loop(0, 2)
    def _(u):
        near(u, 0).wait_recv()
        near(u, 1).wait_recv()
        part = pl.ds(u * upper, upper)
        total = own[part].astype(F32) + near_r[0, part].astype(F32) + near_r[1, part].astype(F32)
        res[part] = total.astype(BF16)

        @pl.loop(jnp.where(u == 0, 1, upper), (u + 1) * upper)
        def _(r):
            give(r).start()

    ret[me] = res[0]

    weights[3].wait()

    def arrived(k):
        return send(ob.at[0, 0], mx.at[k], ob_ss.at[0, 0], ob_rs.at[k], me, p)

    for k in range(4):

        @pl.when(p != k)
        def _():
            arrived(k).wait_recv()

        if k >= 2:

            @pl.when(p == k)
            def _():
                arrived(k).wait_recv()

    projected = dot_t(mx[...].reshape(4 * heads * HD, half // 2), wo[...])
    mix_out[...] = norm_rows(projected, apost_ref[...]).astype(BF16)

    start = pl.multiple_of(p * quarter, quarter)
    own_ids = ids_ref[pl.ds(start, quarter), :]
    own_rw = rw_ref[pl.ds(start, quarter), :]
    each = iota((quarter, experts), 1)
    hit = [own_ids[:, k : k + 1] == each for k in range(TOP_K)]
    lower = (iota((quarter, quarter), 0) > iota((quarter, quarter), 1)).astype(F32).astype(BF16)
    ranks = dot(lower, (hit[0] | hit[1]).astype(F32).astype(BF16))
    slot = iota((quarter, experts * SLOT), 1)
    picks = []
    for k in range(TOP_K):
        rank = jnp.sum(jnp.where(hit[k], ranks, 0.0), axis=1, keepdims=True)
        want = own_ids[:, k : k + 1] * SLOT + rank.astype(jnp.int32)
        picks.append((slot == want).astype(F32).astype(BF16))

    @pl.loop(1, experts)
    def _(r):
        give(r).wait_recv()

    rows_back = ret[...].reshape(experts * SLOT, width)
    combined = jnp.zeros((quarter, width), F32)
    for k in range(TOP_K):
        combined = combined + own_rw[:, k : k + 1] * dot(picks[k], rows_back)
    exp_out[...] = norm_rows(combined, mpost_ref[...]).astype(BF16)

    @pl.loop(1, experts)
    def _(r):
        disp(r, away(r, 1)).wait_send()
        give(r).wait_send()

    @pl.loop(0, experts)
    def _(r):
        fwd(r).wait_send()

    @pl.loop(0, 2)
    def _(u):
        far(u).wait_send()
        near(u, 0).wait_send()
        near(u, 1).wait_send()

    swap.wait_send()
    for part in range(2):
        for d in range(1, 4):
            first(part, d).wait_send()
            for a in range(4):
                second(part, a, d).wait_send()
    for k in range(16):
        third(k).wait_send()
    for q in range(2):
        deliver(1, q).wait_send()

        @pl.when(p != q)
        def _():
            deliver(0, q).wait_send()


def per_device(*args):
    (x, lf, again, wq, wk, wv, wo, apost, m, ids, rw, mgain, wg, wu, wd, mpost) = args
    rows, width = x.shape
    heads, half = wq.shape[1] // HD, rows // 2
    nq = heads * half
    n_ep, n_tp = lax.axis_size("ep"), lax.axis_size("tp")
    units = wg.shape[2]
    upper = n_ep // 2
    tokens = m.shape[0]
    vmem = pl.BlockSpec(memory_space=pltpu.VMEM)
    hbm = pl.BlockSpec(memory_space=pl.ANY)
    dma = pltpu.SemaphoreType.DMA
    row = lambda a: a.reshape(1, -1)
    return pl.pallas_call(
        whole_kernel,
        out_shape=(
            jax.ShapeDtypeStruct((rows // n_tp, width), BF16),
            jax.ShapeDtypeStruct((tokens // n_tp, width), BF16),
        ),
        in_specs=[vmem] * 6 + [hbm, vmem] + [vmem] * 4 + [hbm] * 3 + [vmem],
        out_specs=(vmem, vmem),
        scratch_shapes=[
            pltpu.VMEM((width, units), BF16),
            pltpu.VMEM((width, units), BF16),
            pltpu.VMEM((units, width), BF16),
            pltpu.VMEM(wo.shape, BF16),
            dma((4,)),
            pltpu.VMEM((n_ep, 2, SLOT, width), BF16),
            pltpu.VMEM((2, n_ep, 2, SLOT, width), BF16),
            pltpu.VMEM((upper, 2, SLOT, width), F32),
            pltpu.VMEM((n_ep, SLOT, width), BF16),
            pltpu.VMEM((2, upper, SLOT, width), BF16),
            pltpu.VMEM((2, upper, SLOT, width), BF16),
            pltpu.VMEM((2, 2, upper, SLOT, width), BF16),
            pltpu.VMEM((2, n_ep, SLOT, width), BF16),
            pltpu.VMEM((n_ep, SLOT, width), BF16),
            pltpu.VMEM((n_ep, SLOT, width), BF16),
            pltpu.VMEM((n_ep, 2 * HD, rows), BF16),
            pltpu.VMEM((2, HD, nq), BF16),
            pltpu.VMEM((HD, nq), BF16),
            pltpu.VMEM((n_ep, 16, rows), F32),
            pltpu.VMEM((2, HD + 16, nq), BF16),
            pltpu.VMEM((2, 8, nq), F32),
            pltpu.VMEM((2, HD + 16, nq), F32),
            pltpu.VMEM((2 * half, nq), F32),
            pltpu.VMEM((2 * half, nq), F32),
            pltpu.VMEM((2, 2, heads * HD, half // 2), BF16),
            pltpu.VMEM((4, heads * HD, half // 2), BF16),
            dma((n_ep,)), dma((n_ep,)), dma((n_ep,)), dma((n_ep,)),
            dma((2,)), dma((2,)), dma((2, 2)), dma((2, 2)), dma((n_ep,)), dma((n_ep,)),
            dma((2,)), dma((2, 4)), dma((2, 4)), dma((2, 4, 4)), dma((2, 4, 4)),
            dma((16,)), dma((16,)), dma((2, 2)), dma((4,)),
        ],
        compiler_params=pltpu.CompilerParams(
            has_side_effects=True, vmem_limit_bytes=67_043_328
        ),
        name="whole",
    )(x, lf, row(again), wq, wk, wv, wo, row(apost), m, ids, rw, row(mgain), wg, wu, wd, row(mpost))


def solution(mesh):
    placed = (
        P("ep", None),
        P("tp", None),
        P(),
        P(None, "tp"),
        P(None, "tp"),
        P(None, "tp"),
        P(),
        P(),
        P("ep", None),
        P("ep", None),
        P("ep", None),
        P(),
        P("ep", None, "tp"),
        P("ep", None, "tp"),
        P("ep", "tp", None),
        P(),
    )
    return jax.shard_map(
        per_device,
        mesh=mesh,
        in_specs=placed,
        out_specs=(P(("ep", "tp"), None), P(("ep", "tp"), None)),
        check_vma=False,
    )
```

```python
import functools

import jax
import jax.numpy as jnp
from jax import lax
from jax.experimental import pallas as pl
from jax.experimental.pallas import tpu as pltpu
from jax.sharding import PartitionSpec as P

HD = 64
TOP_K = 2
NEG_FILL = -1e30
NORM_EPS = 1e-06
F32 = jnp.float32
BF16 = jnp.bfloat16
SLOT = 8
SPLIT = 8
FINISH = 4


def norm_rows(values_in, gain_vec):
    widened = values_in.astype(F32)
    return (
        widened
        * lax.rsqrt(jnp.mean(widened * widened, axis=-1, keepdims=True) + NORM_EPS)
        * gain_vec
    )


def dot(a, b):
    return jnp.dot(a, b, preferred_element_type=F32)


def dot_t(a, b):
    return lax.dot_general(a, b, (((0,), (0,)), ((), ())), preferred_element_type=F32)


def iota(shape, dim):
    return lax.broadcasted_iota(jnp.int32, shape, dim)


def whole_kernel(
    x_hbm, lf_ref, again_ref, wq_hbm, wk_hbm, wv_hbm, wo_hbm, apost_ref,
    m_hbm, ids_ref, rw_ref, mgain_ref, wg_hbm, wu_hbm, wd_hbm, mpost_ref,
    mix_out, exp_out,
    x_ref, wq_ref, wk_ref, m_ref, wg, wu, wd, wo, w_sem,
    outgoing, arr, prod, own, far_s, far_r, near_s, near_r, res, ret,
    kv, qo, qf, gs, qs, m_s, acc, s_a, s_b, ob, mx,
    disp_ss, disp_rs, fwd_ss, fwd_rs, far_ss, far_rs, near_ss, near_rs, ret_ss, ret_rs,
    q_sem, k1_ss, k1_rs, k2_ss, k2_rs, k3_ss, k3_rs, ob_ss, ob_rs,
):
    me = lax.axis_index("ep")
    p = lax.axis_index("tp")
    z, y, c = me // 8, (me // 2) % 4, me % 2
    mirror = 31 - me
    parity = p % 2
    rows = x_hbm.shape[0]
    half = rows // 2
    heads = wq_hbm.shape[1] // HD
    nq = heads * half
    width = x_hbm.shape[1]
    tokens = m_hbm.shape[0]
    quarter = tokens // 4
    experts = arr.shape[1]
    upper = experts // 2

    def ep_of(a, b, d):
        return ((a + 8) % 4) * 8 + ((b + 8) % 4) * 2 + (d + 2) % 2

    def away(r, sign):
        g, j, d = r // 8, (r // 2) % 4, r % 2
        return ep_of(z + sign * j, y + sign * (g + j), c + d)

    def send(src, dst, s_sem, r_sem, ep, tp):
        return pltpu.make_async_remote_copy(
            src_ref=src,
            dst_ref=dst,
            send_sem=s_sem,
            recv_sem=r_sem,
            device_id={"ep": ep, "tp": tp},
            device_id_type=pl.DeviceIdType.MESH,
        )

    loads = [
        pltpu.make_async_copy(src, dst, w_sem.at[k])
        for k, (src, dst) in enumerate(
            (
                (m_hbm, m_ref),
                (x_hbm, x_ref),
                (wk_hbm, wk_ref.at[0:HD]),
                (wv_hbm, wk_ref.at[HD : 2 * HD]),
                (wq_hbm, wq_ref),
                (wg_hbm.at[0], wg),
                (wu_hbm.at[0], wu),
                (wd_hbm.at[0], wd),
                (wo_hbm, wo),
            )
        )
    ]
    for load in loads:
        load.start()

    barrier = pltpu.get_barrier_semaphore()

    def greet(ep, tp):
        pl.semaphore_signal(
            barrier, inc=1, device_id={"ep": ep, "tp": tp}, device_id_type=pl.DeviceIdType.MESH
        )

    @pl.loop(1, experts)
    def _(r):
        greet(away(r, 1), p)

    for d in range(1, 4):
        greet(me, (p + d) % 4)
        greet(mirror, (p + d) % 4)

    each = iota((experts, tokens), 0)
    named = [ids_ref[k : k + 1, :] == each for k in range(TOP_K)]
    chosen = named[0] | named[1]
    t_row, t_col = iota((tokens, tokens), 0), iota((tokens, tokens), 1)
    before = ((t_row // quarter == t_col // quarter) & (t_row < t_col)).astype(F32).astype(BF16)
    ranks = dot(chosen.astype(F32).astype(BF16), before)
    ranks_t = jnp.where(chosen, ranks, -1.0)
    block_of = iota((experts, tokens), 1) // quarter
    loads[0].wait()
    normed_m = norm_rows(m_ref[...], mgain_ref[...]).astype(BF16)
    for hb in range(2):
        mine = jnp.where(block_of == parity + 2 * hb, ranks_t, -1.0)
        wide = jnp.broadcast_to(mine[:, None, :], (experts, SLOT, tokens))
        table = jnp.where(wide == iota((experts, SLOT, tokens), 1).astype(F32), 1.0, 0.0)
        table = table.reshape(experts * SLOT, tokens).astype(BF16)
        picked = dot(table, normed_m)
        outgoing[:, hb] = picked.reshape(experts, SLOT, width).astype(BF16)

    def disp(r, peer):
        return send(outgoing.at[peer], arr.at[0, r], disp_ss.at[r], disp_rs.at[r], peer, p)

    def fwd(r):
        return send(
            arr.at[0, r], arr.at[1, r], fwd_ss.at[r], fwd_rs.at[r], me, (p + 1 + 2 * (r % 2)) % 4
        )

    for load in loads[1:5]:
        load.wait()
    normed_a = norm_rows(x_ref[...], again_ref[...]).astype(BF16)
    kv[me] = lax.dot_general(
        wk_ref[...], normed_a, (((1,), (1,)), ((), ())), preferred_element_type=F32
    ).astype(BF16)
    qt = dot(normed_a, wq_ref[...]).astype(BF16).astype(F32) * (HD**-0.5)
    qt = jnp.transpose(qt).astype(BF16)
    for hf in range(2):
        for h in range(heads):
            qo[hf, :, h * half : (h + 1) * half] = qt[
                h * HD : (h + 1) * HD, hf * half : (hf + 1) * half
            ]
    swap = send(qo.at[1], qf, q_sem.at[0], q_sem.at[1], mirror, p)

    def first(part, d):
        ref = kv.at[me, part * HD : (part + 1) * HD]
        to = ep_of(z + d, y, c) if part == 0 else ep_of(z, y + d, c)
        return send(ref, ref, k1_ss.at[part, d], k1_rs.at[part, d], to, p)

    def second(part, a, d):
        owner = ep_of(z - a, y, c) if part == 0 else ep_of(z, y - a, c)
        to = ep_of(z, y + d, c) if part == 0 else ep_of(z + d, y, c)
        ref = kv.at[owner, part * HD : (part + 1) * HD]
        return send(ref, ref, k2_ss.at[part, a, d], k2_rs.at[part, a, d], to, p)

    def third(k):
        ref = kv.at[ep_of(z - k // 4, y - k % 4, c)]
        return send(ref, ref, k3_ss.at[k], k3_rs.at[k], ep_of(z, y, c + 1), p)

    pl.semaphore_wait(barrier, experts - 1 + 6)
    for part in range(2):
        for d in range(1, 4):
            first(part, d).start()

    @pl.loop(1, upper)
    def _(r):
        disp(r, away(r, 1)).start()

    swap.start()
    arr[0, 0] = outgoing[me]

    @pl.loop(0, experts)
    def _(kb):
        rest = -lf_ref[:, pl.ds(pl.multiple_of(kb * rows, rows), rows)]
        for k in range(3):
            piece = rest.astype(BF16).astype(F32)
            gs[kb, k * heads : (k + 1) * heads, :] = piece
            rest = rest - piece
        gs[kb, 3 * heads : 16, :] = jnp.zeros((16 - 3 * heads, rows), F32)

    for part in range(2):
        for a in range(4):
            if a > 0:
                first(part, a).wait_recv()
            for d in range(1, 4):
                second(part, a, d).start()

    @pl.loop(upper, experts)
    def _(r):
        disp(r, away(r, 1)).start()

    fwd(0).start()

    def pass_on(low, high):
        @pl.loop(low, high)
        def _(r):
            disp(r, away(r, 1)).wait_recv()
            fwd(r).start()

    def ffn(v, u):
        rows_in = arr[v, pl.ds(u * upper, upper)].reshape(upper * 2 * SLOT, width)
        gate = dot(rows_in, wg[...])
        up = dot(rows_in, wu[...])
        hidden = (gate / (1.0 + jnp.exp(-gate)) * up).astype(BF16)
        tile = 512

        for n in range(width // tile):
            prod[:, :, :, n * tile : (n + 1) * tile] = dot(
                hidden, wd[:, n * tile : (n + 1) * tile]
            ).reshape(upper, 2, SLOT, tile)

    low = upper // 2

    def far(u, h):
        part = pl.ds(h * low, low)
        return send(
            far_s.at[u, part],
            far_r.at[u, part],
            far_ss.at[u, h],
            far_rs.at[u, h],
            me,
            (p + 1 + 2 * h) % 4,
        )

    def near(u, k, h):
        return send(
            near_s.at[u, k, pl.ds(h * low, low)],
            near_r.at[k, pl.ds(u * upper + h * low, low)],
            near_ss.at[u, k, h],
            near_rs.at[u, k, h],
            me,
            (p + 1 + 2 * k) % 4,
        )

    def direct(u):
        ffn(0, u)
        far_s[u] = prod[:, 1 - p // 2].astype(BF16)
        far(u, 0).start()
        far(u, 1).start()
        own[pl.ds(u * upper, upper)] = prod[:, p // 2].astype(BF16)

    plus = ((p + 1) % 4) // 2

    def passed(u):
        @pl.loop(0, upper)
        def _(k):
            fwd(u * upper + k).wait_recv()

        ffn(1, u)
        for k in range(2):
            h = 1 - k
            near_s[u, k, h * low : (h + 1) * low] = prod[
                h * low : (h + 1) * low, (plus + k) % 2
            ].astype(BF16)
            near(u, k, h).start()
        for k in range(2):
            far(u, k).wait_recv()
            half_of = slice(k * low, (k + 1) * low)
            near_s[u, k, half_of] = (
                prod[half_of, (plus + k) % 2].astype(BF16).astype(F32)
                + far_r[u, half_of].astype(F32)
            ).astype(BF16)
            near(u, k, k).start()

    pass_on(1, upper)
    for load in loads[5:8]:
        load.wait()

    def give(r):
        return send(res.at[r], ret.at[me], ret_ss.at[r], ret_rs.at[r], away(r, -1), p)

    def finish(u):
        for k in range(2):
            for h in range(2):
                near(u, k, h).wait_recv()
        part = pl.ds(u * upper, upper)
        total = own[part].astype(F32) + near_r[0, part].astype(F32) + near_r[1, part].astype(F32)
        res[part] = total.astype(BF16)

        @pl.loop(max(1, u * upper), (u + 1) * upper)
        def _(r):
            give(r).start()

    hidden_keys = iota((half, half), 0) > iota((half, half), 1)

    def place(n):
        late = n >= me
        return jnp.where(late, 1, 0), jnp.where(late, n - me, n)

    def scores(hf, kb, s_ref, mode="full"):
        keys = jnp.concatenate([kv[kb, 0:HD, :].astype(F32), gs[kb]], axis=0)
        keys = jnp.transpose(keys).astype(BF16)
        for pt in [0] if mode == "first" else [0, 1]:
            for h in range(heads):
                cols = slice(h * half, (h + 1) * half)
                s = dot(keys[pt * half : (pt + 1) * half], qs[hf, :, cols])
                if mode == "first" or (mode == "second" and pt == 1):
                    s = jnp.where(hidden_keys, NEG_FILL, s)
                s_ref[pt * half : (pt + 1) * half, cols] = s

    def weigh(hf, kb, s_ref, mode="full"):
        count = half if mode == "first" else 2 * half
        vals = jnp.concatenate([kv[kb, HD : 2 * HD, 0:count], jnp.ones((16, count), BF16)], axis=0)
        for h in range(heads):
            cols = slice(h * half, (h + 1) * half)
            top = m_s[hf, 0:1, cols]
            new = jnp.maximum(top, jnp.max(s_ref[0:count, cols], axis=0, keepdims=True))
            weight = jnp.exp(s_ref[0:count, cols] - new).astype(BF16)
            m_s[hf, 0:1, cols] = new
            acc[hf, :, cols] = acc[hf, :, cols] * jnp.exp(top - new) + dot(vals, weight)

    def attend(t):
        n = 2 * t
        scores(*place(n + 1), s_b)
        weigh(*place(n), s_a)
        scores(*place(n + 2), s_a)
        weigh(*place(n + 1), s_b)

    blocks = (experts - 2) // 2

    @pl.loop(0, 2)
    def _(u):
        direct(u)
        passed(u)

        @pl.when(u == 0)
        def _():
            third(0).start()
            for a in range(4):
                for b in range(4):
                    if (a, b) != (0, 0):
                        if b > 0:
                            second(0, a, b).wait_recv()
                        if a > 0:
                            second(1, b, a).wait_recv()
                        third(a * 4 + b).start()
            swap.wait_recv()
            for k in range(16):
                third(k).wait_recv()

            row, col = iota((16, nq), 0), iota((16, nq), 1)
            sel = jnp.where((row < 3 * heads) & (row % heads == col // half), 1.0, 0.0).astype(BF16)
            qs[0] = jnp.concatenate([qo[0], sel], axis=0)
            qs[1] = jnp.concatenate([qf[...], sel], axis=0)
            m_s[...] = jnp.full(m_s.shape, NEG_FILL, F32)
            acc[...] = jnp.zeros(acc.shape, F32)
            scores(0, me, s_a, "first")
            scores(1, mirror, s_b, "second")
            weigh(0, me, s_a, "first")
            scores(*place(0), s_a)
            weigh(1, mirror, s_b, "second")


        @pl.loop(u * SPLIT, jnp.where(u == 0, SPLIT, blocks))
        def _(t):
            attend(t)

            @pl.when(u == 0)
            def _():
                pass_on(upper + t * upper // SPLIT, upper + (t + 1) * upper // SPLIT)

            @pl.when(t == FINISH)
            def _():
                finish(0)

    weigh(*place(experts - 2), s_a)

    for hf in range(2):
        o = (acc[hf, 0:HD, :] / acc[hf, HD : HD + 1, :]).astype(BF16)
        for q in range(2):
            for h in range(heads):
                ob[hf, q, h * HD : (h + 1) * HD, :] = o[
                    :, h * half + q * (half // 2) : h * half + (q + 1) * (half // 2)
                ]

    def deliver(hf, q):
        return send(
            ob.at[hf, q], mx.at[p], ob_ss.at[hf, q], ob_rs.at[p], me if hf == 0 else mirror, 2 * hf + q
        )

    for q in range(2):
        deliver(1, q).start()

        @pl.when(p == q)
        def _():
            mx[q] = ob[0, q]

        @pl.when(p != q)
        def _():
            deliver(0, q).start()

    finish(1)
    ret[me] = res[0]

    loads[8].wait()

    def arrived(k):
        return send(ob.at[0, 0], mx.at[k], ob_ss.at[0, 0], ob_rs.at[k], me, p)

    for k in range(4):

        @pl.when(p != k)
        def _():
            arrived(k).wait_recv()

        if k >= 2:

            @pl.when(p == k)
            def _():
                arrived(k).wait_recv()

    projected = dot_t(mx[...].reshape(4 * heads * HD, half // 2), wo[...])
    mix_out[...] = norm_rows(projected, apost_ref[...]).astype(BF16)

    mine = (iota((tokens, quarter), 0) == p * quarter + iota((tokens, quarter), 1)).astype(F32).astype(BF16)
    own_ranks = dot(ranks.astype(BF16), mine)
    mine_t = iota((quarter, tokens), 1) == p * quarter + iota((quarter, tokens), 0)
    picks, shares = [], []
    for k in range(TOP_K):
        hit = dot(named[k].astype(F32).astype(BF16), mine)
        want = jnp.where(hit > 0.5, own_ranks, -1.0)
        wide = jnp.broadcast_to(want[:, None, :], (experts, SLOT, quarter))
        table = jnp.where(wide == iota((experts, SLOT, quarter), 1).astype(F32), 1.0, 0.0)
        picks.append(table.reshape(experts * SLOT, quarter).astype(BF16))
        share = jnp.where(mine_t, rw_ref[k : k + 1, :], 0.0)
        shares.append(jnp.sum(share, axis=1, keepdims=True))

    @pl.loop(1, experts)
    def _(r):
        give(r).wait_recv()

    rows_back = ret[...].reshape(experts * SLOT, width)
    combined = jnp.zeros((quarter, width), F32)
    for k in range(TOP_K):
        combined = combined + shares[k] * dot_t(picks[k], rows_back)
    exp_out[...] = norm_rows(combined, mpost_ref[...]).astype(BF16)

    @pl.loop(1, experts)
    def _(r):
        disp(r, away(r, 1)).wait_send()
        give(r).wait_send()

    @pl.loop(0, experts)
    def _(r):
        fwd(r).wait_send()

    @pl.loop(0, 2)
    def _(u):
        for k in range(2):
            far(u, k).wait_send()
            for h in range(2):
                near(u, k, h).wait_send()

    swap.wait_send()
    for part in range(2):
        for d in range(1, 4):
            first(part, d).wait_send()
            for a in range(4):
                second(part, a, d).wait_send()
    for k in range(16):
        third(k).wait_send()
    for q in range(2):
        deliver(1, q).wait_send()

        @pl.when(p != q)
        def _():
            deliver(0, q).wait_send()


def per_device(*args):
    (x, lf, again, wq, wk, wv, wo, apost, m, ids, rw, mgain, wg, wu, wd, mpost) = args
    rows, width = x.shape
    heads, half = wq.shape[1] // HD, rows // 2
    nq = heads * half
    n_ep, n_tp = lax.axis_size("ep"), lax.axis_size("tp")
    units = wg.shape[2]
    upper = n_ep // 2
    tokens = m.shape[0]
    vmem = pl.BlockSpec(memory_space=pltpu.VMEM)
    hbm = pl.BlockSpec(memory_space=pl.ANY)
    dma = pltpu.SemaphoreType.DMA
    row = lambda a: a.reshape(1, -1)
    return pl.pallas_call(
        whole_kernel,
        out_shape=(
            jax.ShapeDtypeStruct((rows // n_tp, width), BF16),
            jax.ShapeDtypeStruct((tokens // n_tp, width), BF16),
        ),
        in_specs=[hbm, vmem, vmem] + [hbm] * 4 + [vmem, hbm] + [vmem] * 3 + [hbm] * 3 + [vmem],
        out_specs=(vmem, vmem),
        scratch_shapes=[
            pltpu.VMEM(x.shape, BF16),
            pltpu.VMEM(wq.shape, BF16),
            pltpu.VMEM((2 * HD, width), BF16),
            pltpu.VMEM(m.shape, BF16),
            pltpu.VMEM((width, units), BF16),
            pltpu.VMEM((width, units), BF16),
            pltpu.VMEM((units, width), BF16),
            pltpu.VMEM(wo.shape, BF16),
            dma((9,)),
            pltpu.VMEM((n_ep, 2, SLOT, width), BF16),
            pltpu.VMEM((2, n_ep, 2, SLOT, width), BF16),
            pltpu.VMEM((upper, 2, SLOT, width), F32),
            pltpu.VMEM((n_ep, SLOT, width), BF16),
            pltpu.VMEM((2, upper, SLOT, width), BF16),
            pltpu.VMEM((2, upper, SLOT, width), BF16),
            pltpu.VMEM((2, 2, upper, SLOT, width), BF16),
            pltpu.VMEM((2, n_ep, SLOT, width), BF16),
            pltpu.VMEM((n_ep, SLOT, width), BF16),
            pltpu.VMEM((n_ep, SLOT, width), BF16),
            pltpu.VMEM((n_ep, 2 * HD, rows), BF16),
            pltpu.VMEM((2, HD, nq), BF16),
            pltpu.VMEM((HD, nq), BF16),
            pltpu.VMEM((n_ep, 16, rows), F32),
            pltpu.VMEM((2, HD + 16, nq), BF16),
            pltpu.VMEM((2, 8, nq), F32),
            pltpu.VMEM((2, HD + 16, nq), F32),
            pltpu.VMEM((2 * half, nq), F32),
            pltpu.VMEM((2 * half, nq), F32),
            pltpu.VMEM((2, 2, heads * HD, half // 2), BF16),
            pltpu.VMEM((4, heads * HD, half // 2), BF16),
            dma((n_ep,)), dma((n_ep,)), dma((n_ep,)), dma((n_ep,)),
            dma((2, 2)), dma((2, 2)), dma((2, 2, 2)), dma((2, 2, 2)), dma((n_ep,)), dma((n_ep,)),
            dma((2,)), dma((2, 4)), dma((2, 4)), dma((2, 4, 4)), dma((2, 4, 4)),
            dma((16,)), dma((16,)), dma((2, 2)), dma((4,)),
        ],
        compiler_params=pltpu.CompilerParams(
            collective_id=0, has_side_effects=True, vmem_limit_bytes=67_043_328
        ),
        name="whole",
    )(x, lf, row(again), wq, wk.T, wv.T, wo, row(apost), m, ids.T, rw.T, row(mgain), wg, wu, wd, row(mpost))


def solution(mesh):
    placed = (
        P("ep", None),
        P("tp", None),
        P(),
        P(None, "tp"),
        P(None, "tp"),
        P(None, "tp"),
        P(),
        P(),
        P("ep", None),
        P("ep", None),
        P("ep", None),
        P(),
        P("ep", None, "tp"),
        P("ep", None, "tp"),
        P("ep", "tp", None),
        P(),
    )
    return jax.shard_map(
        per_device,
        mesh=mesh,
        in_specs=placed,
        out_specs=(P(("ep", "tp"), None), P(("ep", "tp"), None)),
        check_vma=False,
    )
```

```python
import functools

import jax
import jax.numpy as jnp
from jax import lax
from jax.experimental import pallas as pl
from jax.experimental.pallas import tpu as pltpu
from jax.sharding import PartitionSpec as P

HD = 64
TOP_K = 2
NEG_FILL = -1e30
NORM_EPS = 1e-06
F32 = jnp.float32
BF16 = jnp.bfloat16
SLOT = 8
PIECES = 4
FIRST = 1
STARTS = (0, 0, 7, 10)
JOINS = (0, 0, 10, 14)
PUMP = 4
FINISH = (3, 9, 13)


def norm_rows(values_in, gain_vec):
    widened = values_in.astype(F32)
    return (
        widened
        * lax.rsqrt(jnp.mean(widened * widened, axis=-1, keepdims=True) + NORM_EPS)
        * gain_vec
    )


def dot(a, b):
    return jnp.dot(a, b, preferred_element_type=F32)


def dot_t(a, b):
    return lax.dot_general(a, b, (((0,), (0,)), ((), ())), preferred_element_type=F32)


def iota(shape, dim):
    return lax.broadcasted_iota(jnp.int32, shape, dim)


def whole_kernel(
    x_hbm, lf_ref, again_ref, wq_hbm, wk_hbm, wv_hbm, wo_hbm, apost_ref,
    m_hbm, ids_ref, rw_ref, mgain_ref, wg_hbm, wu_hbm, wd_hbm, mpost_ref,
    mix_out, exp_out,
    x_ref, wq_ref, wk_ref, m_ref, wg, wu, wd, wo, w_sem,
    outgoing, arr, prod, own, far_s, far_r, near_s, near_r, res, ret,
    kv, qo, qf, gs, qs, m_s, acc, s_a, s_b, ob, mx,
    disp_ss, disp_rs, fwd_ss, fwd_rs, far_ss, far_rs, near_ss, near_rs, ret_ss, ret_rs,
    q_sem, k1_ss, k1_rs, k2_ss, k2_rs, k3_ss, k3_rs, ob_ss, ob_rs,
):
    me = lax.axis_index("ep")
    p = lax.axis_index("tp")
    z, y, c = me // 8, (me // 2) % 4, me % 2
    mirror = 31 - me
    parity = p % 2
    rows = x_hbm.shape[0]
    half = rows // 2
    heads = wq_hbm.shape[1] // HD
    nq = heads * half
    width = x_hbm.shape[1]
    tokens = m_hbm.shape[0]
    quarter = tokens // 4
    experts = arr.shape[1]
    upper = experts // PIECES
    middle = experts // 2

    def ep_of(a, b, d):
        return ((a + 8) % 4) * 8 + ((b + 8) % 4) * 2 + (d + 2) % 2

    def away(r, sign):
        g, j, d = r // 8, (r // 2) % 4, r % 2
        return ep_of(z + sign * j, y + sign * (g + j), c + d)

    def send(src, dst, s_sem, r_sem, ep, tp):
        return pltpu.make_async_remote_copy(
            src_ref=src,
            dst_ref=dst,
            send_sem=s_sem,
            recv_sem=r_sem,
            device_id={"ep": ep, "tp": tp},
            device_id_type=pl.DeviceIdType.MESH,
        )

    loads = [
        pltpu.make_async_copy(src, dst, w_sem.at[k])
        for k, (src, dst) in enumerate(
            (
                (m_hbm, m_ref),
                (x_hbm, x_ref),
                (wk_hbm, wk_ref.at[0:HD]),
                (wv_hbm, wk_ref.at[HD : 2 * HD]),
                (wq_hbm, wq_ref),
                (wg_hbm.at[0], wg),
                (wu_hbm.at[0], wu),
                (wd_hbm.at[0], wd),
                (wo_hbm, wo),
            )
        )
    ]
    for load in loads:
        load.start()

    barrier = pltpu.get_barrier_semaphore()

    def greet(ep, tp):
        pl.semaphore_signal(
            barrier, inc=1, device_id={"ep": ep, "tp": tp}, device_id_type=pl.DeviceIdType.MESH
        )

    @pl.loop(1, experts)
    def _(r):
        greet(away(r, 1), p)

    for d in range(1, 4):
        greet(me, (p + d) % 4)
        greet(mirror, (p + d) % 4)

    each = iota((experts, tokens), 0)
    named = [ids_ref[k : k + 1, :] == each for k in range(TOP_K)]
    chosen = named[0] | named[1]
    t_row, t_col = iota((tokens, tokens), 0), iota((tokens, tokens), 1)
    before = ((t_row // quarter == t_col // quarter) & (t_row < t_col)).astype(F32).astype(BF16)
    ranks = dot(chosen.astype(F32).astype(BF16), before)
    ranks_t = jnp.where(chosen, ranks, -1.0)
    block_of = iota((experts, tokens), 1) // quarter
    loads[0].wait()
    normed_m = norm_rows(m_ref[...], mgain_ref[...]).astype(BF16)
    for hb in range(2):
        mine = jnp.where(block_of == parity + 2 * hb, ranks_t, -1.0)
        wide = jnp.broadcast_to(mine[:, None, :], (experts, SLOT, tokens))
        table = jnp.where(wide == iota((experts, SLOT, tokens), 1).astype(F32), 1.0, 0.0)
        table = table.reshape(experts * SLOT, tokens).astype(BF16)
        picked = dot(table, normed_m)
        outgoing[:, hb] = picked.reshape(experts, SLOT, width).astype(BF16)

    def disp(r, peer):
        return send(outgoing.at[peer], arr.at[0, r], disp_ss.at[r], disp_rs.at[r], peer, p)

    def fwd(r):
        return send(
            arr.at[0, r], arr.at[1, r], fwd_ss.at[r], fwd_rs.at[r], me, (p + 1 + 2 * (r % 2)) % 4
        )

    for load in loads[1:5]:
        load.wait()
    normed_a = norm_rows(x_ref[...], again_ref[...]).astype(BF16)
    kv[me] = lax.dot_general(
        wk_ref[...], normed_a, (((1,), (1,)), ((), ())), preferred_element_type=F32
    ).astype(BF16)
    qt = dot(normed_a, wq_ref[...]).astype(BF16).astype(F32) * (HD**-0.5)
    qt = jnp.transpose(qt).astype(BF16)
    for hf in range(2):
        for h in range(heads):
            qo[hf, :, h * half : (h + 1) * half] = qt[
                h * HD : (h + 1) * HD, hf * half : (hf + 1) * half
            ]
    swap = send(qo.at[1], qf, q_sem.at[0], q_sem.at[1], mirror, p)

    def first(part, d):
        ref = kv.at[me, part * HD : (part + 1) * HD]
        to = ep_of(z + d, y, c) if part == 0 else ep_of(z, y + d, c)
        return send(ref, ref, k1_ss.at[part, d], k1_rs.at[part, d], to, p)

    def second(part, a, d):
        owner = ep_of(z - a, y, c) if part == 0 else ep_of(z, y - a, c)
        to = ep_of(z, y + d, c) if part == 0 else ep_of(z + d, y, c)
        ref = kv.at[owner, part * HD : (part + 1) * HD]
        return send(ref, ref, k2_ss.at[part, a, d], k2_rs.at[part, a, d], to, p)

    def third(k):
        ref = kv.at[ep_of(z - k // 4, y - k % 4, c)]
        return send(ref, ref, k3_ss.at[k], k3_rs.at[k], ep_of(z, y, c + 1), p)

    pl.semaphore_wait(barrier, experts - 1 + 6)
    for part in range(2):
        for d in range(1, 4):
            first(part, d).start()

    @pl.loop(1, middle)
    def _(r):
        disp(r, away(r, 1)).start()

    swap.start()
    arr[0, 0] = outgoing[me]

    @pl.loop(0, experts)
    def _(kb):
        rest = -lf_ref[:, pl.ds(pl.multiple_of(kb * rows, rows), rows)]
        for k in range(3):
            piece = rest.astype(BF16).astype(F32)
            gs[kb, k * heads : (k + 1) * heads, :] = piece
            rest = rest - piece
        gs[kb, 3 * heads : 16, :] = jnp.zeros((16 - 3 * heads, rows), F32)

    for part in range(2):
        for a in range(4):
            if a > 0:
                first(part, a).wait_recv()
            for d in range(1, 4):
                second(part, a, d).start()

    @pl.loop(middle, experts)
    def _(r):
        disp(r, away(r, 1)).start()

    fwd(0).start()

    def pass_on(low, high):
        @pl.loop(low, high)
        def _(r):
            disp(r, away(r, 1)).wait_recv()
            fwd(r).start()

    def ffn(v, u):
        rows_in = arr[v, pl.ds(u * upper, upper)].reshape(upper * 2 * SLOT, width)
        gate = dot(rows_in, wg[...])
        up = dot(rows_in, wu[...])
        hidden = (gate / (1.0 + jnp.exp(-gate)) * up).astype(BF16)
        tile = 512

        for n in range(width // tile):
            prod[:, :, :, n * tile : (n + 1) * tile] = dot(
                hidden, wd[:, n * tile : (n + 1) * tile]
            ).reshape(upper, 2, SLOT, tile)

    low = upper // 2

    def far(u, h):
        part = pl.ds(h * low, low)
        return send(
            far_s.at[u, part],
            far_r.at[u, part],
            far_ss.at[u, h],
            far_rs.at[u, h],
            me,
            (p + 1 + 2 * h) % 4,
        )

    def near(u, k, h):
        return send(
            near_s.at[u, k, pl.ds(h * low, low)],
            near_r.at[k, pl.ds(u * upper + h * low, low)],
            near_ss.at[u, k, h],
            near_rs.at[u, k, h],
            me,
            (p + 1 + 2 * k) % 4,
        )

    def direct(u):
        ffn(0, u)
        far_s[u] = prod[:, 1 - p // 2].astype(BF16)
        far(u, 0).start()
        far(u, 1).start()
        own[pl.ds(u * upper, upper)] = prod[:, p // 2].astype(BF16)

    plus = ((p + 1) % 4) // 2

    def passed(u):
        @pl.loop(0, upper)
        def _(k):
            fwd(u * upper + k).wait_recv()

        ffn(1, u)
        for k in range(2):
            h = 1 - k
            near_s[u, k, h * low : (h + 1) * low] = prod[
                h * low : (h + 1) * low, (plus + k) % 2
            ].astype(BF16)
            near(u, k, h).start()

    def join(u):
        for k in range(2):
            far(u, k).wait_recv()
            half_of = slice(k * low, (k + 1) * low)
            near_s[u, k, half_of] = (
                prod[half_of, (plus + k) % 2].astype(BF16).astype(F32)
                + far_r[u, half_of].astype(F32)
            ).astype(BF16)
            near(u, k, k).start()

    pass_on(1, upper)
    for load in loads[5:8]:
        load.wait()

    def give(r):
        return send(res.at[r], ret.at[me], ret_ss.at[r], ret_rs.at[r], away(r, -1), p)

    def finish(u):
        for k in range(2):
            for h in range(2):
                near(u, k, h).wait_recv()
        part = pl.ds(u * upper, upper)
        total = own[part].astype(F32) + near_r[0, part].astype(F32) + near_r[1, part].astype(F32)
        res[part] = total.astype(BF16)

        @pl.loop(max(1, u * upper), (u + 1) * upper)
        def _(r):
            give(r).start()

    hidden_keys = iota((half, half), 0) > iota((half, half), 1)

    def place(n):
        late = n >= me
        return jnp.where(late, 1, 0), jnp.where(late, n - me, n)

    def scores(hf, kb, s_ref, mode="full"):
        keys = jnp.concatenate([kv[kb, 0:HD, :].astype(F32), gs[kb]], axis=0)
        keys = jnp.transpose(keys).astype(BF16)
        for pt in [0] if mode == "first" else [0, 1]:
            for h in range(heads):
                cols = slice(h * half, (h + 1) * half)
                s = dot(keys[pt * half : (pt + 1) * half], qs[hf, :, cols])
                if mode == "first" or (mode == "second" and pt == 1):
                    s = jnp.where(hidden_keys, NEG_FILL, s)
                s_ref[pt * half : (pt + 1) * half, cols] = s

    def weigh(hf, kb, s_ref, mode="full"):
        count = half if mode == "first" else 2 * half
        vals = jnp.concatenate([kv[kb, HD : 2 * HD, 0:count], jnp.ones((16, count), BF16)], axis=0)
        for h in range(heads):
            cols = slice(h * half, (h + 1) * half)
            top = m_s[hf, 0:1, cols]
            new = jnp.maximum(top, jnp.max(s_ref[0:count, cols], axis=0, keepdims=True))
            weight = jnp.exp(s_ref[0:count, cols] - new).astype(BF16)
            m_s[hf, 0:1, cols] = new
            acc[hf, :, cols] = acc[hf, :, cols] * jnp.exp(top - new) + dot(vals, weight)

    def attend(t):
        n = 2 * t
        scores(*place(n + 1), s_b)
        weigh(*place(n), s_a)
        scores(*place(n + 2), s_a)
        weigh(*place(n + 1), s_b)

    blocks = (experts - 2) // 2

    def by_piece(u, values):
        out = values[-1]
        for k, v in enumerate(values[:-1]):
            out = jnp.where(u == k, v, out)
        return out

    @pl.loop(0, PIECES)
    def _(u):
        direct(u)

        @pl.when(u == 0)
        def _():
            pass_on(upper, middle)

        passed(u)

        @pl.when(u == FIRST)
        def _():
            third(0).start()
            for a in range(4):
                for b in range(4):
                    if (a, b) != (0, 0):
                        if b > 0:
                            second(0, a, b).wait_recv()
                        if a > 0:
                            second(1, b, a).wait_recv()
                        third(a * 4 + b).start()
            swap.wait_recv()
            for k in range(16):
                third(k).wait_recv()

            row, col = iota((16, nq), 0), iota((16, nq), 1)
            sel = jnp.where((row < 3 * heads) & (row % heads == col // half), 1.0, 0.0).astype(BF16)
            qs[0] = jnp.concatenate([qo[0], sel], axis=0)
            qs[1] = jnp.concatenate([qf[...], sel], axis=0)
            m_s[...] = jnp.full(m_s.shape, NEG_FILL, F32)
            acc[...] = jnp.zeros(acc.shape, F32)
            scores(0, me, s_a, "first")
            scores(1, mirror, s_b, "second")
            weigh(0, me, s_a, "first")
            scores(*place(0), s_a)
            weigh(1, mirror, s_b, "second")


        def attend_from(low_bounds, high_bounds):
            @pl.loop(by_piece(u, low_bounds), by_piece(u, high_bounds))
            def _(t):
                attend(t)

                @pl.when(t < PUMP)
                def _():
                    pass_on(middle + t * middle // PUMP, middle + (t + 1) * middle // PUMP)

                for k, at in enumerate(FINISH):

                    @pl.when(t == at)
                    def _():
                        finish(k)

        attend_from(STARTS, JOINS)
        join(u)
        attend_from(JOINS, STARTS[1:] + ((experts - 2) // 2,))

    weigh(*place(experts - 2), s_a)

    for hf in range(2):
        o = (acc[hf, 0:HD, :] / acc[hf, HD : HD + 1, :]).astype(BF16)
        for q in range(2):
            for h in range(heads):
                ob[hf, q, h * HD : (h + 1) * HD, :] = o[
                    :, h * half + q * (half // 2) : h * half + (q + 1) * (half // 2)
                ]

    def deliver(hf, q):
        return send(
            ob.at[hf, q], mx.at[p], ob_ss.at[hf, q], ob_rs.at[p], me if hf == 0 else mirror, 2 * hf + q
        )

    for q in range(2):
        deliver(1, q).start()

        @pl.when(p == q)
        def _():
            mx[q] = ob[0, q]

        @pl.when(p != q)
        def _():
            deliver(0, q).start()

    finish(PIECES - 1)
    ret[me] = res[0]

    loads[8].wait()

    def arrived(k):
        return send(ob.at[0, 0], mx.at[k], ob_ss.at[0, 0], ob_rs.at[k], me, p)

    for k in range(4):

        @pl.when(p != k)
        def _():
            arrived(k).wait_recv()

        if k >= 2:

            @pl.when(p == k)
            def _():
                arrived(k).wait_recv()

    projected = dot_t(mx[...].reshape(4 * heads * HD, half // 2), wo[...])
    mix_out[...] = norm_rows(projected, apost_ref[...]).astype(BF16)

    mine = (iota((tokens, quarter), 0) == p * quarter + iota((tokens, quarter), 1)).astype(F32).astype(BF16)
    own_ranks = dot(ranks.astype(BF16), mine)
    mine_t = iota((quarter, tokens), 1) == p * quarter + iota((quarter, tokens), 0)
    picks, shares = [], []
    for k in range(TOP_K):
        hit = dot(named[k].astype(F32).astype(BF16), mine)
        want = jnp.where(hit > 0.5, own_ranks, -1.0)
        wide = jnp.broadcast_to(want[:, None, :], (experts, SLOT, quarter))
        table = jnp.where(wide == iota((experts, SLOT, quarter), 1).astype(F32), 1.0, 0.0)
        picks.append(table.reshape(experts * SLOT, quarter).astype(BF16))
        share = jnp.where(mine_t, rw_ref[k : k + 1, :], 0.0)
        shares.append(jnp.sum(share, axis=1, keepdims=True))

    @pl.loop(1, experts)
    def _(r):
        give(r).wait_recv()

    rows_back = ret[...].reshape(experts * SLOT, width)
    combined = jnp.zeros((quarter, width), F32)
    for k in range(TOP_K):
        combined = combined + shares[k] * dot_t(picks[k], rows_back)
    exp_out[...] = norm_rows(combined, mpost_ref[...]).astype(BF16)

    @pl.loop(1, experts)
    def _(r):
        disp(r, away(r, 1)).wait_send()
        give(r).wait_send()

    @pl.loop(0, experts)
    def _(r):
        fwd(r).wait_send()

    @pl.loop(0, PIECES)
    def _(u):
        for k in range(2):
            far(u, k).wait_send()
            for h in range(2):
                near(u, k, h).wait_send()

    swap.wait_send()
    for part in range(2):
        for d in range(1, 4):
            first(part, d).wait_send()
            for a in range(4):
                second(part, a, d).wait_send()
    for k in range(16):
        third(k).wait_send()
    for q in range(2):
        deliver(1, q).wait_send()

        @pl.when(p != q)
        def _():
            deliver(0, q).wait_send()


def put_out(a_ref, b_ref, a_out, b_out, sems):
    copies = [
        pltpu.make_async_copy(a_ref, a_out, sems.at[0]),
        pltpu.make_async_copy(b_ref, b_out, sems.at[1]),
    ]
    for copy in copies:
        copy.start()
    for copy in copies:
        copy.wait()


def per_device(*args):
    (x, lf, again, wq, wk, wv, wo, apost, m, ids, rw, mgain, wg, wu, wd, mpost) = args
    rows, width = x.shape
    heads, half = wq.shape[1] // HD, rows // 2
    nq = heads * half
    n_ep, n_tp = lax.axis_size("ep"), lax.axis_size("tp")
    units = wg.shape[2]
    upper = n_ep // PIECES
    tokens = m.shape[0]
    vmem = pl.BlockSpec(memory_space=pltpu.VMEM)
    hbm = pl.BlockSpec(memory_space=pl.ANY)
    dma = pltpu.SemaphoreType.DMA
    row = lambda a: a.reshape(1, -1)
    results = pl.pallas_call(
        whole_kernel,
        out_shape=(
            jax.ShapeDtypeStruct((rows // n_tp, width), BF16),
            jax.ShapeDtypeStruct((tokens // n_tp, width), BF16),
        ),
        in_specs=[hbm, vmem, vmem] + [hbm] * 4 + [vmem, hbm] + [vmem] * 3 + [hbm] * 3 + [vmem],
        out_specs=(vmem, vmem),
        scratch_shapes=[
            pltpu.VMEM(x.shape, BF16),
            pltpu.VMEM(wq.shape, BF16),
            pltpu.VMEM((2 * HD, width), BF16),
            pltpu.VMEM(m.shape, BF16),
            pltpu.VMEM((width, units), BF16),
            pltpu.VMEM((width, units), BF16),
            pltpu.VMEM((units, width), BF16),
            pltpu.VMEM(wo.shape, BF16),
            dma((9,)),
            pltpu.VMEM((n_ep, 2, SLOT, width), BF16),
            pltpu.VMEM((2, n_ep, 2, SLOT, width), BF16),
            pltpu.VMEM((upper, 2, SLOT, width), F32),
            pltpu.VMEM((n_ep, SLOT, width), BF16),
            pltpu.VMEM((PIECES, upper, SLOT, width), BF16),
            pltpu.VMEM((PIECES, upper, SLOT, width), BF16),
            pltpu.VMEM((PIECES, 2, upper, SLOT, width), BF16),
            pltpu.VMEM((2, n_ep, SLOT, width), BF16),
            pltpu.VMEM((n_ep, SLOT, width), BF16),
            pltpu.VMEM((n_ep, SLOT, width), BF16),
            pltpu.VMEM((n_ep, 2 * HD, rows), BF16),
            pltpu.VMEM((2, HD, nq), BF16),
            pltpu.VMEM((HD, nq), BF16),
            pltpu.VMEM((n_ep, 16, rows), F32),
            pltpu.VMEM((2, HD + 16, nq), BF16),
            pltpu.VMEM((2, 8, nq), F32),
            pltpu.VMEM((2, HD + 16, nq), F32),
            pltpu.VMEM((2 * half, nq), F32),
            pltpu.VMEM((2 * half, nq), F32),
            pltpu.VMEM((2, 2, heads * HD, half // 2), BF16),
            pltpu.VMEM((4, heads * HD, half // 2), BF16),
            dma((n_ep,)), dma((n_ep,)), dma((n_ep,)), dma((n_ep,)),
            dma((PIECES, 2)), dma((PIECES, 2)), dma((PIECES, 2, 2)), dma((PIECES, 2, 2)), dma((n_ep,)), dma((n_ep,)),
            dma((2,)), dma((2, 4)), dma((2, 4)), dma((2, 4, 4)), dma((2, 4, 4)),
            dma((16,)), dma((16,)), dma((2, 2)), dma((4,)),
        ],
        compiler_params=pltpu.CompilerParams(
            collective_id=0, has_side_effects=True, vmem_limit_bytes=67_043_328
        ),
        name="whole",
    )(x, lf, row(again), wq, wk.T, wv.T, wo, row(apost), m, ids.T, rw.T, row(mgain), wg, wu, wd, row(mpost))
    return pl.pallas_call(
        put_out,
        out_shape=tuple(jax.ShapeDtypeStruct(r.shape, r.dtype) for r in results),
        in_specs=[vmem, vmem],
        out_specs=(hbm, hbm),
        scratch_shapes=[dma((2,))],
        name="put_out",
    )(*results)


def solution(mesh):
    placed = (
        P("ep", None),
        P("tp", None),
        P(),
        P(None, "tp"),
        P(None, "tp"),
        P(None, "tp"),
        P(),
        P(),
        P("ep", None),
        P("ep", None),
        P("ep", None),
        P(),
        P("ep", None, "tp"),
        P("ep", None, "tp"),
        P("ep", "tp", None),
        P(),
    )
    return jax.shard_map(
        per_device,
        mesh=mesh,
        in_specs=placed,
        out_specs=(P(("ep", "tp"), None), P(("ep", "tp"), None)),
        check_vma=False,
    )
```
